32 devices in a mesh: grp: 2 (over y), sp: 8 (over z, core), tp: 2 (over x).
Axes of the slice: x: 2, y: 2, z: 4, core: 2. Of those that a mesh axis runs over, the one named last changes fastest.
Arguments:
- queries: bfloat16 [12288, 1024], P(('grp', 'sp'), 'tp'), parts along dimension 0, may hold values from -200 to 200
- key_rows: bfloat16 [12288, 512], P(('grp', 'sp'), 'tp'), parts along dimension 0, may hold values from -6 to 6
- value_rows: bfloat16 [12288, 512], P(('grp', 'sp'), 'tp'), parts along dimension 0, may hold values from -6 to 6
- doc_ids: int32 [12288], P(('grp', 'sp')), parts along dimension 0, may hold values from 0 to 3, never falling along the last dimension, each value on 1 to 3072 neighbouring positions
- sink_logits: float32 [16], P('tp'), may hold values from 2 to 7
- out_weight: bfloat16 [1024, 2048], P('tp', 'sp'), may hold values from -0.1875 to 0.1875
- residual: bfloat16 [12288, 2048], P(('grp', 'sp', 'tp')), parts along dimension 0, may hold values from -6 to 6
- gain_mixed: float32 [2048], replicated, may hold values from 0.1 to 1.9
- gain_before: float32 [2048], replicated, may hold values from 0.1 to 1.9
- gain_after: float32 [2048], replicated, may hold values from 0.1 to 1.9
- gate_weight: bfloat16 [2048, 6144], P('sp', 'tp'), may hold values from -0.125 to 0.125
- up_weight: bfloat16 [2048, 6144], P('sp', 'tp'), may hold values from -0.125 to 0.125
- down_weight: bfloat16 [6144, 2048], P('tp', 'sp'), may hold values from -0.078125 to 0.078125
Outputs:
- layer_out: bfloat16 [12288, 2048], P(('grp', 'sp', 'tp')), parts along dimension 0
The draws below stay inside these ranges and needn't reach their ends.
There are 2 independent parts, one for each index of `grp`. The reference program is written for one: setup_inputs(seed, part) draws one part's arguments, and reference() takes and returns one part's arrays. A program takes and returns all parts, laid end to end along the dimension named above; an argument that names none is the same for every part. Nothing has to cross between parts.
All inputs are finite; a program needn't handle non-finite values.
Results may differ from the reference program's by a relative error of at most 0.015.
Values may be sent and summed in bfloat16 or wider, within the bound.
A program may use at most 128 MiB of HBM per device.

```python
import math
import jax
import jax.numpy as jnp
import numpy as np
from jax import lax

D = 2048
HEADS = 16
KV_HEADS = 8
HEAD_DIM = 64
FF = 6144
WINDOW = 128
TOKENS = 6144
DOCS = 4
DOC_MOST = 3072
N_TP = 2


def drawn(key):
    base_keys = jnp.clip(jax.random.normal(jax.random.fold_in(key, 11), (TOKENS, KV_HEADS * HEAD_DIM), jnp.float32), -5.0, 5.0)
    base_queries = jnp.clip(jax.random.normal(jax.random.fold_in(key, 12), (TOKENS, HEADS * HEAD_DIM), jnp.float32), -5.0, 5.0)
    return (base_queries, base_keys)


def draw_queries(key, part):
    return drawn(key)[0].astype(jnp.bfloat16)


def draw_key_rows(key, part):
    return drawn(key)[1].astype(jnp.bfloat16)


def shard_levels(key, dims, pieces, smallest, top_value):
    level, own = 1.0, jax.random.fold_in(key, 6)
    for axis_at, blocks in pieces:
        heights = jnp.exp(jax.random.uniform(jax.random.fold_in(own, axis_at), (blocks,), jnp.float32, smallest / len(pieces), top_value / len(pieces)))
        level = level * jnp.repeat(heights, dims[axis_at] // blocks).reshape([-1 if axis == axis_at else 1 for axis in range(len(dims))])
    return level


def length_profile(amount, total, bound, skew):
    weights = [(1 << 20) // math.isqrt(rank ** skew) + 1 for rank in range(2, amount + 1)]
    spare, holding = total - bound - (amount - 1), [1] * (amount - 1)
    while spare > 0:
        candidates = [i for i in range(amount - 1) if holding[i] < bound]
        mass, remaining = sum([weights[i] for i in candidates]), spare
        for i in candidates:
            more = min(bound - holding[i], max(1, remaining * weights[i] // mass), spare)
            holding[i] = holding[i] + more
            spare = spare - more
    return np.array([bound] + holding)


def uneven_parts(stream_key, count, total, bound, skew):
    if count == 2:
        one = jax.random.randint(stream_key, (), max(1, total - bound), min(bound, total - 1) + 1)
        return jnp.stack([one, total - one])
    lengths = jnp.asarray(length_profile(count, total, bound, skew), jnp.int32)
    twos = (count - 1) // 2
    source_of, taker = lengths[1:1 + 2 * twos:2], lengths[2:2 + 2 * twos:2]
    margin = jnp.minimum(source_of - 1, bound - taker)
    moved = jax.random.randint(jax.random.fold_in(stream_key, 1), (twos,), 0, 1 << 20) % (margin + 1)
    lengths = lengths.at[1:1 + 2 * twos:2].set(source_of - moved).at[2:2 + 2 * twos:2].set(taker + moved)
    return lengths[jax.random.permutation(jax.random.fold_in(stream_key, 2), count)]


def centred(stream_key, dims, width, most, split=(), kind=jnp.bfloat16):
    level = shard_levels(stream_key, dims, split, -0.22, 0.18) if split else 1.0
    drawn = jax.random.normal(stream_key, dims, jnp.float32) * width * level
    return jnp.minimum(jnp.maximum(drawn, -most), most).astype(kind)


def setup_inputs(seed: int = 0, part: int = 0) -> dict:
    arg_keys = jax.random.split(jax.random.key(seed), 14)
    own_keys = jax.random.split(jax.random.fold_in(arg_keys[13], part), 14)
    return {
        "queries": draw_queries(jax.random.fold_in(jax.random.fold_in(arg_keys[13], part), 71), part),
        "key_rows": draw_key_rows(jax.random.fold_in(jax.random.fold_in(arg_keys[13], part), 71), part),
        "value_rows": centred(own_keys[2], (TOKENS, KV_HEADS * HEAD_DIM), 1.0, 6.0, ((0, 8), (1, 2))),
        "doc_ids": jnp.searchsorted(jnp.cumsum(uneven_parts(own_keys[3], DOCS, TOKENS, DOC_MOST, 1)), jnp.arange(TOKENS), side="right").astype(jnp.int32),
        "sink_logits": jnp.clip(2.0 + 5.0 * jax.random.uniform(arg_keys[4], (HEADS,), jnp.float32) ** shard_levels(arg_keys[4], (HEADS,), ((0, 2),), -0.2, 0.2), 2.0, 7.0),
        "out_weight": centred(arg_keys[5], (HEADS * HEAD_DIM, D), (HEADS * HEAD_DIM) ** -0.5, 0.1875, ((0, 2), (1, 8))),
        "residual": centred(own_keys[6], (TOKENS, D), 1.0, 6.0, ((0, 16),)),
        "gain_mixed": jnp.clip(1.0 + 0.18 * jax.random.normal(arg_keys[7], (D,), jnp.float32), 0.1, 1.9),
        "gain_before": jnp.clip(1.0 + 0.18 * jax.random.normal(arg_keys[8], (D,), jnp.float32), 0.1, 1.9),
        "gain_after": jnp.clip(1.0 + 0.18 * jax.random.normal(arg_keys[9], (D,), jnp.float32), 0.1, 1.9),
        "gate_weight": centred(arg_keys[10], (D, FF), D ** -0.5, 0.125, ((0, 8), (1, 2))),
        "up_weight": centred(arg_keys[11], (D, FF), D ** -0.5, 0.125, ((0, 8), (1, 2))),
        "down_weight": centred(arg_keys[12], (FF, D), FF ** -0.5, 0.078125, ((0, 2), (1, 8))),
    }


epsilon = 1e-06
masked_value = -1e+30

def stored(value):
    return lax.optimization_barrier(value.astype(jnp.bfloat16)).astype(jnp.float32)

def rms_scaled(value, gain):
    return value * lax.rsqrt(lax.optimization_barrier(jnp.mean(value * value, axis=-1, keepdims=True)) + epsilon) * gain

def reference(queries, key_rows, value_rows, doc_ids, sink_logits, out_weight, residual, gain_mixed, gain_before, gain_after, gate_weight, up_weight, down_weight):
    total = queries.shape[0]
    blocks = total // WINDOW
    group_size = HEADS // KV_HEADS
    padded_keys = jnp.concatenate([jnp.zeros((WINDOW, KV_HEADS * HEAD_DIM), jnp.bfloat16), key_rows], axis=0)
    padded_values = jnp.concatenate([jnp.zeros((WINDOW, KV_HEADS * HEAD_DIM), jnp.bfloat16), value_rows], axis=0)
    padded_docs = jnp.concatenate([jnp.zeros((WINDOW,), jnp.int32) - 1, doc_ids], axis=0)
    key_pos = jnp.arange(total + WINDOW, dtype=jnp.int32) - WINDOW

    def windows(array):
        first = array[:-WINDOW].reshape((blocks, WINDOW) + array.shape[1:])
        second = array[WINDOW:].reshape((blocks, WINDOW) + array.shape[1:])
        return jnp.concatenate([first, second], axis=1)
    key_blocks = windows(padded_keys).reshape(blocks, 2 * WINDOW, KV_HEADS, HEAD_DIM).astype(jnp.float32)
    value_blocks = windows(padded_values).reshape(blocks, 2 * WINDOW, KV_HEADS, HEAD_DIM).astype(jnp.float32)
    key_docs = windows(padded_docs)
    key_places = windows(key_pos)
    query_blocks = queries.reshape(blocks, WINDOW, KV_HEADS, group_size, HEAD_DIM).astype(jnp.float32)
    query_places = jnp.arange(total, dtype=jnp.int32).reshape(blocks, WINDOW)
    query_docs = doc_ids.reshape(blocks, WINDOW)
    scores = jnp.einsum('bqhgd,bkhd->bhgqk', query_blocks, key_blocks) * HEAD_DIM ** (-0.5)
    distance = query_places[:, :, None] - key_places[:, None, :]
    valid = (distance >= 0) & (distance < WINDOW) & (key_places[:, None, :] >= 0)
    valid = valid & (query_docs[:, :, None] == key_docs[:, None, :])
    scores = jnp.where(valid[:, None, None], scores, masked_value)
    sinks = sink_logits.reshape(KV_HEADS, group_size)[None, :, :, None]
    top = jnp.maximum(lax.optimization_barrier(jnp.max(scores, axis=-1)), sinks)
    weight = jnp.exp(scores - top[..., None])
    denom = lax.optimization_barrier(jnp.sum(weight, axis=-1)) + jnp.exp(sinks - top)
    weight_b = weight.astype(jnp.bfloat16).astype(jnp.float32)
    summed = jnp.einsum('bhgqk,bkhd->bqhgd', weight_b, value_blocks)
    scale = jnp.transpose(denom, (0, 3, 1, 2))[..., None]
    mixed = (summed / scale).reshape(total, HEADS * HEAD_DIM).astype(jnp.bfloat16)
    projected = stored(jnp.dot(mixed, out_weight, preferred_element_type=jnp.float32))
    after = stored(residual.astype(jnp.float32) + rms_scaled(projected, gain_mixed))
    normed = rms_scaled(after, gain_before).astype(jnp.bfloat16)
    gate = jnp.dot(normed, gate_weight, preferred_element_type=jnp.float32)
    upward = jnp.dot(normed, up_weight, preferred_element_type=jnp.float32)
    hidden = (jax.nn.silu(gate) * upward).astype(jnp.bfloat16)
    block_size = FF // N_TP
    summed_out = jnp.zeros((total, D), jnp.float32)
    for index in range(N_TP):
        partial_sum = jnp.dot(hidden[:, index * block_size:(index + 1) * block_size], down_weight[index * block_size:(index + 1) * block_size], preferred_element_type=jnp.float32)
        summed_out = summed_out + stored(partial_sum)
    ffn_out = stored(summed_out)
    return (after + 0.5 * rms_scaled(ffn_out, gain_after)).astype(jnp.bfloat16)
```

```python
import functools

import jax
import jax.numpy as jnp
from jax import lax
from jax.experimental import pallas as pl
from jax.experimental.pallas import tpu as pltpu
from jax.sharding import PartitionSpec as P

HEAD_DIM = 64
WINDOW = 128


epsilon = 1e-06
masked_value = -1e30


def passed_along(value, axis, steps):
    count = lax.axis_size(axis)
    first, last = (max(0, -steps), min(count, count - steps))
    return lax.ppermute(value, axis, [(source, source + steps) for source in range(first, last)])


def stored(value):
    return lax.optimization_barrier(value.astype(jnp.bfloat16)).astype(jnp.float32)


def rms_scaled(value, gain):
    return value * lax.rsqrt(jnp.mean(value * value, axis=-1, keepdims=True) + epsilon) * gain


def windows(array, blocks):
    first = array[:-WINDOW].reshape((blocks, WINDOW) + array.shape[1:])
    second = array[WINDOW:].reshape((blocks, WINDOW) + array.shape[1:])
    return jnp.concatenate([first, second], axis=1)


def attend(queries, key_rows, value_rows, doc_ids, sink_logits):
    length = queries.shape[0]
    blocks = length // WINDOW
    local_kv = key_rows.shape[1] // HEAD_DIM
    group_size = queries.shape[1] // HEAD_DIM // local_kv
    offset = lax.axis_index("sp") * length
    tail_keys, tail_values, tail_docs = passed_along(
        (key_rows[length - WINDOW :], value_rows[length - WINDOW :], doc_ids[length - WINDOW :]),
        "sp",
        1,
    )
    key_blocks = windows(jnp.concatenate([tail_keys, key_rows], axis=0), blocks).reshape(
        blocks, 2 * WINDOW, local_kv, HEAD_DIM
    )
    value_blocks = windows(jnp.concatenate([tail_values, value_rows], axis=0), blocks).reshape(
        blocks, 2 * WINDOW, local_kv, HEAD_DIM
    )
    key_docs = windows(jnp.concatenate([tail_docs, doc_ids], axis=0), blocks)
    key_places = windows(offset - WINDOW + jnp.arange(length + WINDOW, dtype=jnp.int32), blocks)
    query_places = (offset + jnp.arange(length, dtype=jnp.int32)).reshape(blocks, WINDOW)
    query_docs = doc_ids.reshape(blocks, WINDOW)
    query_blocks = queries.reshape(blocks, WINDOW, local_kv, group_size, HEAD_DIM)
    scores = jnp.einsum(
        "bqhgd,bkhd->bhgqk", query_blocks, key_blocks, preferred_element_type=jnp.float32
    ) * HEAD_DIM ** (-0.5)
    distance = query_places[:, :, None] - key_places[:, None, :]
    valid = (distance >= 0) & (distance < WINDOW) & (key_places[:, None, :] >= 0)
    valid = valid & (query_docs[:, :, None] == key_docs[:, None, :])
    scores = jnp.where(valid[:, None, None], scores, masked_value)
    sinks = sink_logits.reshape(local_kv, group_size)[None, :, :, None]
    top = jnp.maximum(jnp.max(scores, axis=-1), sinks)
    weight = jnp.exp(scores - top[..., None])
    denom = jnp.sum(weight, axis=-1) + jnp.exp(sinks - top)
    summed = jnp.einsum(
        "bhgqk,bkhd->bqhgd",
        weight.astype(jnp.bfloat16),
        value_blocks,
        preferred_element_type=jnp.float32,
    )
    scale = jnp.transpose(denom, (0, 3, 1, 2))[..., None]
    return (summed / scale).reshape(length, queries.shape[1]).astype(jnp.bfloat16)

MESH = pl.DeviceIdType.MESH
PHASES = 4


def block_kernel(
    levels, mixed, wout, resid, gain_m, gain_b, gain_a, gate, up, down, out,
    full_gate, full_up, full_down, psend, precv, after, normed, hidden, fsend, frecv, fown,
    z_recv, z_up, z_dn, y_send, y_recv, c_send, c_recv, own_sem, x_send, x_recv, f_send, f_recv,
):
    y, s, x = lax.axis_index("grp"), lax.axis_index("sp"), lax.axis_index("tp")
    z, c = s // 2, s % 2
    y_peer, x_peer, c_peer = {"grp": 1 - y}, {"tp": 1 - x}, {"sp": z * 2 + 1 - c}
    above, below = {"sp": jnp.minimum(s + 2, 2 * levels - 1)}, {"sp": jnp.maximum(s - 2, 0)}
    half_rows = gate.shape[0] // 2
    down_rows = down.shape[0] // 2
    width = down.shape[1] // 2
    mine = resid.shape[0]
    dim = resid.shape[1]
    own_rows, peer_rows = pl.ds(pl.multiple_of(x * mine, mine), mine), pl.ds(pl.multiple_of((1 - x) * mine, mine), mine)

    barrier = pltpu.get_barrier_semaphore()

    def greet(device):
        pl.semaphore_signal(barrier, inc=1, device_id=device, device_id_type=MESH)

    greet(y_peer)
    greet(x_peer)
    greet(c_peer)

    @pl.when(z < levels - 1)
    def _():
        greet(above)

    @pl.when(z > 0)
    def _():
        greet(below)

    neighbours = jnp.where(z > 0, 1, 0) + jnp.where(z < levels - 1, 1, 0)
    pl.semaphore_wait(barrier, 3 + neighbours)

    def place(q, zz, cc, hh):
        if q < 2:
            row = pl.multiple_of(((zz * 2 + cc) * 2 + hh) * half_rows, half_rows)
            return (full_gate, full_up)[q].at[pl.ds(row, half_rows), :]
        return full_down.at[
            q - 2, zz, pl.ds(pl.multiple_of(hh * down_rows, down_rows), down_rows), pl.ds(pl.multiple_of(cc * width, width), width)
        ]

    def piece(q, hh):
        if q < 2:
            return (gate, up)[q].at[pl.ds(pl.multiple_of(hh * half_rows, half_rows), half_rows), :]
        return down.at[pl.ds(pl.multiple_of(hh * down_rows, down_rows), down_rows), pl.ds((q - 2) * width, width)]

    def remote(source, target, send, recv, device):
        return pltpu.make_async_remote_copy(
            src_ref=source, dst_ref=target, send_sem=send, recv_sem=recv, device_id=device, device_id_type=MESH
        )

    def upward(q, zz, source):
        return remote(source, place(q, zz, c, y), z_up.at[q, zz], z_recv.at[q, zz], above)

    def downward(q, zz, source):
        return remote(source, place(q, zz, c, y), z_dn.at[q, zz], z_recv.at[q, zz], below)

    def across(q, zz):
        block = place(q, zz, c, y)
        return remote(block, block, y_send.at[q, zz], y_recv.at[q, zz], y_peer)

    def arrived_across(q, zz):
        block = place(q, zz, c, 1 - y)
        return remote(block, block, y_send.at[q, zz], y_recv.at[q, zz], y_peer)

    def beside(q, zz, hh, cc, source=None):
        block = place(q, zz, cc, hh)
        return remote(block if source is None else source, block, c_send.at[q, zz, hh], c_recv.at[q, zz, hh], c_peer)

    def keep(q, hh):
        return pltpu.make_async_copy(piece(q, hh), place(q, z, c, hh), own_sem.at[q, hh])

    def own(q):
        @pl.when(z < levels - 1)
        def _():
            upward(q, z, piece(q, y)).start()

        @pl.when(z > 0)
        def _():
            downward(q, z, piece(q, y)).start()

        for hh in range(2):
            beside(q, z, hh, c, piece(q, hh)).start()
            keep(q, hh).start()

    def from_line(q, t):
        low, high = z - t, z + t

        @pl.when(low >= 0)
        def _():
            upward(q, low, place(q, low, c, y)).wait_recv()

            @pl.when(z < levels - 1)
            def _():
                upward(q, low, place(q, low, c, y)).start()

            across(q, low).start()
            beside(q, low, y, c).start()

        @pl.when(high < levels)
        def _():
            downward(q, high, place(q, high, c, y)).wait_recv()

            @pl.when(z > 0)
            def _():
                downward(q, high, place(q, high, c, y)).start()

            across(q, high).start()
            beside(q, high, y, c).start()

    def from_side(q, t):
        for zz, there in ((z - t, z - t >= 0), (z + t, z + t < levels)):

            @pl.when(there)
            def _(zz=zz):
                arrived_across(q, zz).wait_recv()
                beside(q, zz, 1 - y, c).start()

    def from_partner(q, zz):
        for hh in range(2):
            beside(q, zz, hh, 1 - c).wait_recv()

    def project():
        def tile(j, _):
            cols = pl.ds(pl.multiple_of(j * 256, 256), 256)
            psend[:, cols] = jnp.dot(mixed[peer_rows, :], wout[:, cols], preferred_element_type=jnp.float32).astype(jnp.bfloat16)
            out[:, cols] = jnp.dot(mixed[own_rows, :], wout[:, cols], preferred_element_type=jnp.float32).astype(jnp.bfloat16)
            return 0

        lax.fori_loop(0, dim // 256, tile, 0)

    def sent_projection():
        return remote(psend, precv, x_send.at[0], x_recv.at[0], x_peer)

    def sent_normed(rows):
        return remote(normed.at[rows, :], normed.at[rows, :], x_send.at[1], x_recv.at[1], x_peer)

    step_rows = 32

    def norms():
        def tile(i, _):
            rows = pl.ds(pl.multiple_of(i * step_rows, step_rows), step_rows)
            projected = (out[rows, :].astype(jnp.float32) + precv[rows, :].astype(jnp.float32)).astype(jnp.bfloat16).astype(jnp.float32)
            total = (resid[rows, :].astype(jnp.float32) + rms_scaled(projected, gain_m[...])).astype(jnp.bfloat16)
            after[rows, :] = total
            placed = pl.ds(pl.multiple_of(x * mine + i * step_rows, step_rows), step_rows)
            normed[placed, :] = rms_scaled(total.astype(jnp.float32), gain_b[...]).astype(jnp.bfloat16)
            return 0

        lax.fori_loop(0, mine // step_rows, tile, 0)

    tiles = full_gate.shape[1] // 256

    def gathered(w):
        for hh in range(2):
            keep(w, hh).wait()
        for zz in range(levels):
            from_partner(w, zz)

    def gated(first, last):
        def tile(j, _):
            cols = pl.ds(pl.multiple_of(j * 256, 256), 256)
            g = jnp.dot(normed[...], full_gate[:, cols], preferred_element_type=jnp.float32)
            hidden[:, cols] = (g / (1.0 + jnp.exp(-g))).astype(jnp.bfloat16)
            return 0

        lax.fori_loop(first, last, tile, 0)

    def raised(first, last):
        def tile(j, _):
            cols = pl.ds(pl.multiple_of(j * 256, 256), 256)
            u = jnp.dot(normed[...], full_up[:, cols], preferred_element_type=jnp.float32)
            hidden[:, cols] = (hidden[:, cols].astype(jnp.float32) * u).astype(jnp.bfloat16)
            return 0

        lax.fori_loop(first, last, tile, 0)

    def sent_sum(k, zz):
        return remote(fsend.at[k, zz], frecv.at[k, zz], f_send.at[k, zz], f_recv.at[k, zz], x_peer)

    def lowered(k, zz):
        from_partner(k + 2, zz)
        block = full_down.at[k, zz]
        fsend[k, zz] = jnp.dot(hidden[peer_rows, :], block[...], preferred_element_type=jnp.float32).astype(jnp.bfloat16)
        sent_sum(k, zz).start()
        fown[k, zz] = jnp.dot(hidden[own_rows, :], block[...], preferred_element_type=jnp.float32).astype(jnp.bfloat16)

    def lowered_ring(k, t):
        def one(side, _):
            zz = z - t + 2 * t * side

            @pl.when((zz >= 0) & (zz < levels))
            def _():
                lowered(k, zz)

            return 0

        lax.fori_loop(0, 2, one, 0)

    own(0)
    own(1)
    project()
    sent_projection().start()
    previous = None
    second_gate = (levels - 1) + min(2, levels - 1) - 1
    second_up = second_gate + levels - 1
    last_tick = PHASES * (levels - 1) - 1
    for q in range(PHASES):
        for t in range(1, levels):
            from_line(q, t)
            if previous is not None:
                from_side(*previous)
            previous = (q, t)
            if q == 0 and t == 1:
                own(2)
            if q == 0 and t == min(2, levels - 1):
                sent_projection().wait()
                norms()
                sent_normed(own_rows).start()
            if q == 1 and t == 1:
                own(3)
            tick = q * (levels - 1) + t - 1
            if tick == second_gate:
                sent_normed(own_rows).wait_send()
                sent_normed(peer_rows).wait_recv()
                gathered(0)
            if second_gate <= tick < second_up:
                at, spread = tick - second_gate, second_up - second_gate
                gated(tiles * at // spread, tiles * (at + 1) // spread)
            if tick == second_up:
                gathered(1)
            if second_up <= tick < last_tick:
                at, spread = tick - second_up, last_tick - second_up
                raised(tiles * at // spread, tiles * (at + 1) // spread)
            if tick == last_tick:
                for w in (2, 3):
                    for hh in range(2):
                        keep(w, hh).wait()

                def first_half(zz, _):
                    lowered(0, zz)
                    return 0

                lax.fori_loop(0, levels, first_half, 0)
                lowered(1, z)
                for near in range(1, levels - 1):
                    lowered_ring(1, near)
    from_side(*previous)
    lowered_ring(1, levels - 1)

    def drain(zz, _):
        for k in range(2):
            sent_sum(k, zz).wait()
        for q in range(PHASES):
            for hh in range(2):
                beside(q, zz, hh, c).wait_send()

            @pl.when((zz <= z) & (z < levels - 1))
            def _(q=q):
                upward(q, zz, place(q, zz, c, y)).wait_send()

            @pl.when((zz >= z) & (z > 0))
            def _(q=q):
                downward(q, zz, place(q, zz, c, y)).wait_send()

            @pl.when(zz != z)
            def _(q=q):
                across(q, zz).wait_send()

        return 0

    lax.fori_loop(0, levels, drain, 0)

    def finish(i, _):
        rows = pl.ds(pl.multiple_of(i * step_rows, step_rows), step_rows)
        parts = [
            fown[k, zz, rows, cc * width : (cc + 1) * width].astype(jnp.float32)
            + frecv[k, zz, rows, cc * width : (cc + 1) * width].astype(jnp.float32)
            for zz in range(levels)
            for cc in range(2)
            for k in range(2)
        ]
        ffn_out = jnp.concatenate(parts, axis=1).astype(jnp.bfloat16).astype(jnp.float32)
        out[rows, :] = (after[rows, :].astype(jnp.float32) + 0.5 * rms_scaled(ffn_out, gain_a[...])).astype(jnp.bfloat16)
        return 0

    lax.fori_loop(0, mine // step_rows, finish, 0)


def fused(mixed, head_columns, residual, gain_mixed, gain_before, gain_after, gate_weight, up_weight, down_weight):
    levels = lax.axis_size("sp") // 2
    rows, dim = mixed.shape[0], residual.shape[1]
    mine = residual.shape[0]
    hidden = gate_weight.shape[1]
    half = down_weight.shape[1] // 2
    vmem, whole = pl.BlockSpec(memory_space=pltpu.VMEM), pl.BlockSpec(memory_space=pl.ANY)
    bf16, dma = jnp.bfloat16, pltpu.SemaphoreType.DMA
    return pl.pallas_call(
        functools.partial(block_kernel, levels),
        out_shape=jax.ShapeDtypeStruct((mine, dim), bf16),
        in_specs=[vmem] * 6 + [whole] * 3,
        out_specs=vmem,
        scratch_shapes=[
            pltpu.VMEM((dim, hidden), bf16),
            pltpu.VMEM((dim, hidden), bf16),
            pltpu.VMEM((2, levels, hidden, 2 * half), bf16),
            pltpu.VMEM((mine, dim), bf16),
            pltpu.VMEM((mine, dim), bf16),
            pltpu.VMEM((mine, dim), bf16),
            pltpu.VMEM((rows, dim), bf16),
            pltpu.VMEM((rows, hidden), bf16),
            pltpu.VMEM((2, levels, mine, 2 * half), bf16),
            pltpu.VMEM((2, levels, mine, 2 * half), bf16),
            pltpu.VMEM((2, levels, mine, 2 * half), bf16),
            dma((PHASES, levels)),
            dma((PHASES, levels)),
            dma((PHASES, levels)),
            dma((PHASES, levels)),
            dma((PHASES, levels)),
            dma((PHASES, levels, 2)),
            dma((PHASES, levels, 2)),
            dma((PHASES, 2)),
            dma((2,)),
            dma((2,)),
            dma((2, levels)),
            dma((2, levels)),
        ],
        compiler_params=pltpu.CompilerParams(collective_id=0, has_side_effects=True, vmem_limit_bytes=67043328),
    )(
        mixed, head_columns, residual, gain_mixed[None], gain_before[None], gain_after[None],
        gate_weight, up_weight, down_weight,
    )


def per_device(
    queries,
    key_rows,
    value_rows,
    doc_ids,
    sink_logits,
    out_weight,
    residual,
    gain_mixed,
    gain_before,
    gain_after,
    gate_weight,
    up_weight,
    down_weight,
):
    mixed = attend(queries, key_rows, value_rows, doc_ids, sink_logits)
    head_columns = lax.all_gather(out_weight, "sp", axis=1, tiled=True)
    pairs = lax.axis_size("grp") == 2 and lax.axis_size("tp") == 2
    if pairs and lax.axis_size("sp") % 2 == 0 and lax.axis_size("sp") >= 4:
        return fused(
            mixed, head_columns, residual, gain_mixed, gain_before, gain_after, gate_weight, up_weight, down_weight
        )
    projected = lax.psum_scatter(
        jnp.dot(mixed, head_columns, preferred_element_type=jnp.float32).astype(jnp.bfloat16),
        "tp",
        scatter_dimension=0,
        tiled=True,
    ).astype(jnp.float32)
    projected = stored(projected)
    after = stored(residual.astype(jnp.float32) + rms_scaled(projected, gain_mixed))
    normed = rms_scaled(after, gain_before).astype(jnp.bfloat16)
    full_gate, full_up, full_down = (
        lax.all_gather(gate_weight, "sp", axis=0, tiled=True),
        lax.all_gather(up_weight, "sp", axis=0, tiled=True),
        lax.all_gather(down_weight, "sp", axis=1, tiled=True),
    )
    piece = lax.all_gather(normed, "tp", axis=0, tiled=True)
    gate = jnp.dot(piece, full_gate, preferred_element_type=jnp.float32)
    upward = jnp.dot(piece, full_up, preferred_element_type=jnp.float32)
    hidden = (jax.nn.silu(gate) * upward).astype(jnp.bfloat16)
    ffn_out = stored(
        lax.psum_scatter(
            jnp.dot(hidden, full_down, preferred_element_type=jnp.float32).astype(jnp.bfloat16),
            "tp",
            scatter_dimension=0,
            tiled=True,
        ).astype(jnp.float32)
    )
    return (after + 0.5 * rms_scaled(ffn_out, gain_after)).astype(jnp.bfloat16)


def solution(mesh):
    return jax.shard_map(
        per_device,
        mesh=mesh,
        in_specs=(
            P(("grp", "sp"), "tp"),
            P(("grp", "sp"), "tp"),
            P(("grp", "sp"), "tp"),
            P(("grp", "sp")),
            P("tp"),
            P("tp", "sp"),
            P(("grp", "sp", "tp"), None),
            P(),
            P(),
            P(),
            P("sp", "tp"),
            P("sp", "tp"),
            P("tp", "sp"),
        ),
        out_specs=P(("grp", "sp", "tp"), None),
        check_vma=False,
    )
```
